32 devices in a mesh: kv: 8 (over z, x), tp: 4 (over y, core).
Axes of the slice: x: 2, y: 2, z: 4, core: 2. Of those that a mesh axis runs over, the one named last changes fastest.
Arguments:
- tokens: bfloat16 [8, 4096], P(None, 'kv'), may hold values from -15 to 15
- norm_gain: float32 [4096], P('kv'), may hold values from 0.1 to 1.9
- w_query: bfloat16 [4096, 2048], P('kv', 'tp'), may hold values from -0.09375 to 0.09375
- w_key: bfloat16 [4096, 2048], P('kv', 'tp'), may hold values from -0.09375 to 0.09375
- w_value: bfloat16 [4096, 2048], P('kv', 'tp'), may hold values from -0.09375 to 0.09375
- w_forget: bfloat16 [4096, 32], P('kv', 'tp'), may hold values from -0.09375 to 0.09375
- forget_bias: float32 [32], P('tp'), may hold values from -1 to 3
- key_cache: bfloat16 [8, 3072, 2048], P(None, 'kv', 'tp'), may hold values from -360 to 360
- value_cache: bfloat16 [8, 3072, 2048], P(None, 'kv', 'tp'), may hold values from -6 to 6
- gate_cache: float32 [8, 32, 3072], P(None, 'tp', 'kv'), may hold values from -3072 to 0, as said below
- lengths: int32 [8], replicated, may hold values from 1536 to 3072, as said below
- w_out: bfloat16 [2048, 4096], P('tp', 'kv'), may hold values from -0.125 to 0.125
Outputs:
- mixed: bfloat16 [8, 4096], P(None, ('kv', 'tp'))
- log_total: float32 [8, 32], P(None, 'tp')
The draws below stay inside these ranges and needn't reach their ends.
Inputs may be any that keep to these rules, and one draw needn't show every extreme that they name: `lengths`: the largest length equals 3072. `gate_cache`: never increasing along positions.
All inputs are finite; a program needn't handle non-finite values.
Results may differ from the reference program's by a relative error of at most 0.014.
Values may be sent and summed in bfloat16 or wider, within the bound.
A program may use at most 64 MiB of HBM per device.

```python
import jax
import jax.numpy as jnp
from jax import lax

D = 4096
HEADS = 32
HEAD = 64
BATCH = 8
POS_DEV = 384
LENGTH = 3072
N_KV = 8
N_TP = 4


def draw_tokens(key, part):
    first, second = jax.random.split(key, 2)
    blocks = D // 64
    scales = jnp.exp(jax.random.uniform(second, (1, blocks), jnp.float32, jnp.log(0.4), jnp.log(2.5)))
    scales = jnp.repeat(scales, 64, axis=1)
    values = jnp.clip(jax.random.normal(first, (BATCH, D), jnp.float32), -6.0, 6.0)
    return (values * scales).astype(jnp.bfloat16)


def draw_key_cache(key, part):
    first, second = jax.random.split(key, 2)
    values = jnp.clip(jax.random.normal(first, (BATCH, LENGTH, HEADS * HEAD), jnp.float32), -6.0, 6.0)
    return values.astype(jnp.bfloat16)


def draw_gate_cache(key, part):
    first, second, third = jax.random.split(key, 3)
    order = jax.random.permutation(first, HEADS)
    fast = order < HEADS // 2
    base = jnp.where(fast, 0.08, 1.5 / LENGTH)
    block = jnp.exp(jax.random.uniform(second, (BATCH, HEADS, LENGTH // 64), jnp.float32, jnp.log(0.4), jnp.log(2.5)))
    block = jnp.repeat(block, 64, axis=2)
    rough = jax.random.uniform(third, (BATCH, HEADS, LENGTH), jnp.float32, 0.5, 1.5)
    step = base[None, :, None] * block * rough
    return -jnp.cumsum(step, axis=-1)


def draw_lengths(key, part):
    first, second = jax.random.split(key, 2)
    values = jax.random.randint(first, (BATCH,), LENGTH // 2, LENGTH + 1)
    longest = jax.random.randint(second, (), 0, BATCH)
    return jnp.where(jnp.arange(BATCH) == longest, LENGTH, values).astype(jnp.int32)


def block_scale(own_key, dims, cuts, least, top_value):
    loudness, own = 1.0, jax.random.fold_in(own_key, 6)
    for axis_at, parts in cuts:
        draws = jnp.exp(jax.random.uniform(jax.random.fold_in(own, axis_at), (parts,), jnp.float32, least / len(cuts), top_value / len(cuts)))
        loudness = loudness * jnp.repeat(draws, dims[axis_at] // parts).reshape([-1 if axis == axis_at else 1 for axis in range(len(dims))])
    return loudness


def gaussian(stream_key, dims, scale, most, cuts=(), kind=jnp.bfloat16):
    loudness = block_scale(stream_key, dims, cuts, -0.22, 0.18) if cuts else 1.0
    result = jax.random.normal(stream_key, dims, jnp.float32) * scale * loudness
    return jnp.minimum(jnp.maximum(result, -most), most).astype(kind)


def setup_inputs(seed: int = 0) -> dict:
    splits = jax.random.split(jax.random.key(seed), 13)
    return {
        "tokens": draw_tokens(jax.random.fold_in(splits[12], 71), 0),
        "norm_gain": jnp.clip(1.0 + 0.18 * jax.random.normal(splits[1], (D,), jnp.float32), 0.1, 1.9),
        "w_query": gaussian(splits[2], (D, HEADS * HEAD), D ** -0.5, 0.09375, ((0, 8), (1, 4))),
        "w_key": gaussian(splits[3], (D, HEADS * HEAD), D ** -0.5, 0.09375, ((0, 8), (1, 4))),
        "w_value": gaussian(splits[4], (D, HEADS * HEAD), D ** -0.5, 0.09375, ((0, 8), (1, 4))),
        "w_forget": gaussian(splits[5], (D, HEADS), D ** -0.5, 0.09375, ((0, 8), (1, 4))),
        "forget_bias": jnp.clip(-1.0 + 4.0 * jax.random.uniform(splits[6], (HEADS,), jnp.float32) ** block_scale(splits[6], (HEADS,), ((0, 4),), -0.2, 0.2), -1.0, 3.0),
        "key_cache": draw_key_cache(jax.random.fold_in(splits[12], 71), 0),
        "value_cache": gaussian(splits[8], (BATCH, LENGTH, HEADS * HEAD), 1.0, 6.0, ((1, 8), (2, 4))),
        "gate_cache": draw_gate_cache(jax.random.fold_in(splits[12], 71), 0),
        "lengths": draw_lengths(jax.random.fold_in(splits[12], 71), 0),
        "w_out": gaussian(splits[11], (HEADS * HEAD, D), (HEADS * HEAD) ** -0.5, 0.125, ((0, 4), (1, 8))),
    }


EPS = 1e-06
MASKED = -1e+30

def cache_blocks(args):
    query, keys, values, gates, valid = args
    heads = query.shape[0]
    width = query.shape[1]
    keys_four = keys.astype(jnp.float32).reshape(N_KV, POS_DEV, heads, width)
    values_four = values.astype(jnp.float32).reshape(N_KV, POS_DEV, heads, width)
    score = jnp.einsum('he,nphe->hnp', query.astype(jnp.float32), keys_four) * HEAD ** (-0.5)
    score = score - gates.reshape(heads, N_KV, POS_DEV)
    usable = valid.reshape(1, N_KV, POS_DEV)
    score = jnp.where(usable, score, MASKED)
    block_max = lax.optimization_barrier(jnp.max(score, axis=-1))
    weights = jnp.where(usable, jnp.exp(score - block_max[..., None]), 0.0)
    block_sum = lax.optimization_barrier(jnp.sum(weights, axis=-1))
    weights_low = lax.optimization_barrier(weights.astype(jnp.bfloat16))
    block_acc = jnp.einsum('hnp,nphe->hne', weights_low.astype(jnp.float32), values_four)
    cache_max = lax.optimization_barrier(jnp.max(block_max, axis=-1))
    factor = jnp.exp(block_max - cache_max[:, None])
    return (cache_max, lax.optimization_barrier(jnp.sum(block_sum * factor, axis=-1)), lax.optimization_barrier(jnp.sum(block_acc * factor[..., None], axis=1)))

def reference(tokens, norm_gain, w_query, w_key, w_value, w_forget, forget_bias, key_cache, value_cache, gate_cache, lengths, w_out):
    wide = tokens.astype(jnp.float32)
    scaled = (wide * norm_gain).astype(jnp.bfloat16)
    rstd = lax.rsqrt(lax.optimization_barrier(jnp.mean(wide * wide, axis=-1)) + EPS)[:, None]
    query = (jnp.dot(scaled, w_query, preferred_element_type=jnp.float32) * rstd).astype(jnp.bfloat16)
    key_new = (jnp.dot(scaled, w_key, preferred_element_type=jnp.float32) * rstd).astype(jnp.bfloat16)
    value_new = (jnp.dot(scaled, w_value, preferred_element_type=jnp.float32) * rstd).astype(jnp.bfloat16)
    log_gate = jax.nn.log_sigmoid(jnp.dot(scaled, w_forget, preferred_element_type=jnp.float32) * rstd + forget_bias)
    positions = jnp.arange(LENGTH, dtype=jnp.int32)
    valid = positions[None, :] < lengths[:, None]
    last = (positions[None, :] == lengths[:, None] - 1)[:, None, :]
    gate_now = lax.optimization_barrier(jnp.sum(jnp.where(last, gate_cache, 0.0), axis=-1)) + log_gate
    query_heads = query.reshape(BATCH, HEADS, HEAD)
    cache_max, cache_sum, cache_acc = lax.map(cache_blocks, (query_heads, key_cache, value_cache, gate_cache, valid))
    self_score = lax.optimization_barrier(jnp.sum(query_heads.astype(jnp.float32) * key_new.reshape(BATCH, HEADS, HEAD).astype(jnp.float32), axis=-1)) * HEAD ** (-0.5)
    cache_top = cache_max + gate_now
    top = jnp.maximum(cache_top, self_score)
    cache_factor = jnp.exp(cache_top - top)
    self_factor = jnp.exp(self_score - top)
    total = cache_sum * cache_factor + self_factor
    attended = (cache_acc * cache_factor[..., None] + self_factor[..., None] * value_new.reshape(BATCH, HEADS, HEAD).astype(jnp.float32)) / total[..., None]
    attended = attended.reshape(BATCH, HEADS * HEAD).astype(jnp.bfloat16)
    log_total = top + jnp.log(total)
    group_rows = HEADS * HEAD // N_TP
    partial_value = jnp.einsum('btk,tkd->btd', attended.reshape(BATCH, N_TP, group_rows).astype(jnp.float32), w_out.reshape(N_TP, group_rows, D).astype(jnp.float32))
    partial_value = partial_value.astype(jnp.bfloat16).astype(jnp.float32)
    mixed = lax.optimization_barrier(jnp.sum(partial_value, axis=1)).astype(jnp.bfloat16)
    return (mixed, log_total)
```

```python
import functools

import jax
import jax.numpy as jnp
from jax import lax
from jax.experimental import pallas as pl
from jax.experimental.pallas import tpu as pltpu
from jax.sharding import PartitionSpec as P

EPS = 1e-06
MASKED = -1e30
F32 = jnp.float32
BF16 = jnp.bfloat16


def exchange(axis, me, n, buf, send_sem, recv_sem):
    for d in range(1, n):
        pltpu.make_async_remote_copy(
            src_ref=buf.at[me],
            dst_ref=buf.at[me],
            send_sem=send_sem.at[d - 1],
            recv_sem=recv_sem.at[d - 1],
            device_id={axis: lax.rem(me + d, n)},
            device_id_type=pl.DeviceIdType.MESH,
        ).start()


def arrived(axis, me, n, buf, send_sem, recv_sem):
    for d in range(1, n):
        slot = lax.rem(me + n - d, n)
        pltpu.make_async_remote_copy(
            src_ref=buf.at[slot],
            dst_ref=buf.at[slot],
            send_sem=send_sem.at[d - 1],
            recv_sem=recv_sem.at[d - 1],
            device_id={axis: slot},
            device_id_type=pl.DeviceIdType.MESH,
        ).wait_recv()


def left(axis, me, n, buf, send_sem, recv_sem):
    for d in range(1, n):
        pltpu.make_async_remote_copy(
            src_ref=buf.at[me],
            dst_ref=buf.at[me],
            send_sem=send_sem.at[d - 1],
            recv_sem=recv_sem.at[d - 1],
            device_id={axis: lax.rem(me + d, n)},
            device_id_type=pl.DeviceIdType.MESH,
        ).wait_send()


def kernel(n, t, features, lengths, tokens_h, gain_h, wq_h, wk_h, wv_h, wf_h, bias_h, key_h, value_h, gate_h, wo_h,
           mixed, log_total, tokens, gain, wq, wk, wv, wf, bias, key, value, gate, wo,
           proj, pval, stats, acc, outs, inbox,
           in_sem, proj_s, proj_r, pval_s, pval_r, stats_s, stats_r, acc_s, acc_r, out_s, out_r):
    me = lax.axis_index("kv")
    mt = lax.axis_index("tp")
    batch, heads, positions = gate.shape
    width = wq.shape[1]
    size = width // heads

    pairs = [(tokens_h, tokens), (gain_h, gain), (wq_h, wq), (wf_h, wf), (wv_h, wv), (wk_h, wk), (gate_h, gate),
             (bias_h, bias), (key_h, key), (value_h, value), (wo_h, wo)]
    copies = [pltpu.make_async_copy(a, b, in_sem.at[i]) for i, (a, b) in enumerate(pairs)]
    (c_tok, c_gain, c_wq, c_wf, c_wv, c_wk, c_gate, c_bias, c_key, c_value, c_wo) = copies
    for c in copies:
        c.start()

    barrier = pltpu.get_barrier_semaphore()
    for d in range(1, n):
        pl.semaphore_signal(barrier, inc=1, device_id={"kv": lax.rem(me + d, n)}, device_id_type=pl.DeviceIdType.MESH)
    for d in range(1, t):
        pl.semaphore_signal(barrier, inc=1, device_id={"tp": lax.rem(mt + d, t)}, device_id_type=pl.DeviceIdType.MESH)

    c_tok.wait()
    c_gain.wait()
    wide = tokens[...].astype(F32)
    scaled = (wide * gain[...]).astype(BF16)
    square = jnp.sum(wide * wide, axis=-1, keepdims=True)
    c_wq.wait()
    c_wf.wait()
    proj[me, :, :width] = jnp.dot(scaled, wq[...], preferred_element_type=F32)
    proj[me, :, width:] = jnp.broadcast_to(square, (batch, 128))
    proj[me, :, width : width + heads] = lax.dot_general(
        scaled, wf[...], (((1,), (1,)), ((), ())), preferred_element_type=F32)
    pl.semaphore_wait(barrier, n - 1 + t - 1)
    proj_x = ("kv", me, n, proj, proj_s, proj_r)
    exchange(*proj_x)

    c_wv.wait()
    pval[me] = jnp.dot(scaled, wv[...], preferred_element_type=F32).astype(BF16)
    pval_x = ("kv", me, n, pval, pval_s, pval_r)
    exchange(*pval_x)
    c_wk.wait()
    part_key = jnp.dot(scaled, wk[...], preferred_element_type=F32)
    c_gate.wait()
    c_bias.wait()
    c_key.wait()

    arrived(*proj_x)
    summed = jnp.sum(proj[...], axis=0)
    rstd = lax.rsqrt(summed[:, width + heads : width + heads + 1] / features + EPS)
    query = (summed[:, :width] * rstd).astype(BF16).astype(F32)
    forget = summed[:, width : width + heads] * rstd + bias[...]
    log_gate = jnp.minimum(forget, 0.0) - jnp.log1p(jnp.exp(-jnp.abs(forget)))

    row = lax.broadcasted_iota(jnp.int32, (heads, width), 0)
    col = lax.broadcasted_iota(jnp.int32, (heads, width), 1)
    own = (col >= row * size) & (col < (row + 1) * size)
    place = me * positions + lax.broadcasted_iota(jnp.int32, (heads, positions), 1)
    h_row = lax.broadcasted_iota(jnp.int32, (heads, 128), 0)
    lane = lax.broadcasted_iota(jnp.int32, (heads, 128), 1)
    scale = size ** -0.5
    c_value.wait()
    rows, sums = [], []
    for b in range(batch):
        spread = jnp.where(own, query[b : b + 1, :], 0.0)
        score = lax.dot_general(spread.astype(BF16), key[b], (((1,), (1,)), ((), ())), preferred_element_type=F32) * scale
        g = gate[b]
        usable = place < lengths[b]
        score = jnp.where(usable, score - g, MASKED)
        top = jnp.max(score, axis=-1, keepdims=True)
        weights = jnp.where(usable, jnp.exp(score - top), 0.0)
        total = jnp.sum(weights, axis=-1, keepdims=True)
        last = jnp.sum(jnp.where(place == lengths[b] - 1, g, 0.0), axis=-1, keepdims=True)
        own_score = jnp.sum(spread * part_key[b : b + 1, :], axis=-1, keepdims=True)
        tile = jnp.where(lane == h_row, top, 0.0)
        tile = jnp.where(lane == h_row + heads, total, tile)
        tile = jnp.where(lane == h_row + 2 * heads, last, tile)
        tile = jnp.where(lane == h_row + 3 * heads, own_score, tile)
        sums.append(jnp.sum(tile, axis=0, keepdims=True))
        full = jnp.dot(weights.astype(BF16), value[b], preferred_element_type=F32)
        rows.append(jnp.sum(jnp.where(own, full, 0.0), axis=0, keepdims=True))
    stats[me] = jnp.concatenate(sums, axis=0)
    acc[me] = jnp.concatenate(rows, axis=0).astype(BF16)
    stats_x = ("kv", me, n, stats, stats_s, stats_r)
    acc_x = ("kv", me, n, acc, acc_s, acc_r)
    exchange(*stats_x)
    exchange(*acc_x)

    arrived(*pval_x)
    value_new = jnp.sum(pval[...].astype(F32), axis=0)
    arrived(*stats_x)
    st = stats[...]
    tops = st[:, :, :heads]
    cache_max = jnp.max(tops, axis=0)
    factor = jnp.exp(tops - cache_max[None])
    cache_sum = jnp.sum(factor * st[:, :, heads : 2 * heads], axis=0)
    gate_now = jnp.sum(st[:, :, 2 * heads : 3 * heads], axis=0) + log_gate
    self_score = jnp.sum(st[:, :, 3 * heads : 4 * heads], axis=0) * rstd * scale
    cache_top = cache_max + gate_now
    top = jnp.maximum(cache_top, self_score)
    cache_factor = jnp.exp(cache_top - top)
    self_factor = jnp.exp(self_score - top)
    total = cache_sum * cache_factor + self_factor
    log_total[...] = top + jnp.log(total)
    inverse = 1.0 / total
    each = factor * (cache_factor * inverse)[None]
    coef = jnp.concatenate([each.reshape(n * batch, heads), self_factor * inverse * rstd], axis=0)
    wide_coef = jnp.dot(coef, own.astype(F32), precision=lax.Precision.HIGHEST, preferred_element_type=F32)
    arrived(*acc_x)
    attended = wide_coef[n * batch :] * value_new + jnp.sum(
        wide_coef[: n * batch].reshape(n, batch, width) * acc[...].astype(F32), axis=0)
    c_wo.wait()
    partial = jnp.dot(attended.astype(BF16), wo[...], preferred_element_type=F32).astype(BF16)
    cols = partial.shape[1] // t
    for i in range(t):
        outs[i] = partial[:, i * cols : (i + 1) * cols]
    for d in range(1, t):
        peer = lax.rem(mt + d, t)
        pltpu.make_async_remote_copy(
            src_ref=outs.at[peer], dst_ref=inbox.at[mt], send_sem=out_s.at[d - 1], recv_sem=out_r.at[d - 1],
            device_id={"tp": peer}, device_id_type=pl.DeviceIdType.MESH).start()
    inbox[mt] = outs[mt]
    left(*proj_x)
    left(*pval_x)
    left(*stats_x)
    left(*acc_x)
    for d in range(1, t):
        slot = lax.rem(mt + t - d, t)
        pltpu.make_async_remote_copy(
            src_ref=outs.at[slot], dst_ref=inbox.at[slot], send_sem=out_s.at[d - 1], recv_sem=out_r.at[d - 1],
            device_id={"tp": slot}, device_id_type=pl.DeviceIdType.MESH).wait()
    mixed[...] = jnp.sum(inbox[...].astype(F32), axis=0).astype(BF16)


def body(n, t, tokens, norm_gain, w_query, w_key, w_value, w_forget, forget_bias, key_cache, value_cache, gate_cache,
         lengths, w_out):
    batch = tokens.shape[0]
    heads = gate_cache.shape[1]
    width = w_query.shape[1]
    cols = w_out.shape[1] // t
    arrays = (tokens, norm_gain.reshape(1, -1), w_query, w_key, w_value, w_forget.T, forget_bias.reshape(1, -1),
              key_cache, value_cache, gate_cache, w_out)
    dma = pltpu.SemaphoreType.DMA
    return pl.pallas_call(
        functools.partial(kernel, n, t, float(tokens.shape[1] * n)),
        out_shape=(
            jax.ShapeDtypeStruct((batch, cols), BF16),
            jax.ShapeDtypeStruct((batch, heads), F32),
        ),
        in_specs=[pl.BlockSpec(memory_space=pltpu.SMEM)] + [pl.BlockSpec(memory_space=pl.ANY)] * len(arrays),
        out_specs=(pl.BlockSpec(memory_space=pltpu.VMEM), pl.BlockSpec(memory_space=pltpu.VMEM)),
        scratch_shapes=[pltpu.VMEM(a.shape, a.dtype) for a in arrays] + [
            pltpu.VMEM((n, batch, width + 128), F32),
            pltpu.VMEM((n, batch, width), BF16),
            pltpu.VMEM((n, batch, 128), F32),
            pltpu.VMEM((n, batch, width), BF16),
            pltpu.VMEM((t, batch, cols), BF16),
            pltpu.VMEM((t, batch, cols), BF16),
            dma((len(arrays),)),
        ] + [dma((n - 1,))] * 8 + [dma((t - 1,))] * 2,
        compiler_params=pltpu.CompilerParams(collective_id=0, has_side_effects=True),
    )(lengths, *arrays)


def solution(mesh):
    placed = (
        P(None, "kv"),
        P("kv"),
        P("kv", "tp"),
        P("kv", "tp"),
        P("kv", "tp"),
        P("kv", "tp"),
        P("tp"),
        P(None, "kv", "tp"),
        P(None, "kv", "tp"),
        P(None, "tp", "kv"),
        P(),
        P("tp", "kv"),
    )
    return jax.shard_map(
        functools.partial(body, mesh.shape["kv"], mesh.shape["tp"]),
        mesh=mesh,
        in_specs=placed,
        out_specs=(P(None, ("kv", "tp")), P(None, "tp")),
        check_vma=False,
    )
```

```python
import functools

import jax
import jax.numpy as jnp
from jax import lax
from jax.experimental import pallas as pl
from jax.experimental.pallas import tpu as pltpu
from jax.sharding import PartitionSpec as P

EPS = 1e-06
MASKED = -1e30
F32 = jnp.float32
BF16 = jnp.bfloat16


def exchange(axis, me, n, buf, send_sem, recv_sem):
    for d in range(1, n):
        pltpu.make_async_remote_copy(
            src_ref=buf.at[me],
            dst_ref=buf.at[me],
            send_sem=send_sem.at[d - 1],
            recv_sem=recv_sem.at[d - 1],
            device_id={axis: lax.rem(me + d, n)},
            device_id_type=pl.DeviceIdType.MESH,
        ).start()


def arrived(axis, me, n, buf, send_sem, recv_sem):
    for d in range(1, n):
        slot = lax.rem(me + n - d, n)
        pltpu.make_async_remote_copy(
            src_ref=buf.at[slot],
            dst_ref=buf.at[slot],
            send_sem=send_sem.at[d - 1],
            recv_sem=recv_sem.at[d - 1],
            device_id={axis: slot},
            device_id_type=pl.DeviceIdType.MESH,
        ).wait_recv()


def left(axis, me, n, buf, send_sem, recv_sem):
    for d in range(1, n):
        pltpu.make_async_remote_copy(
            src_ref=buf.at[me],
            dst_ref=buf.at[me],
            send_sem=send_sem.at[d - 1],
            recv_sem=recv_sem.at[d - 1],
            device_id={axis: lax.rem(me + d, n)},
            device_id_type=pl.DeviceIdType.MESH,
        ).wait_send()


def kernel(n, t, features, lengths, tokens_h, gain_h, wq_h, wk_h, wv_h, wf_h, bias_h, key_h, value_h, gate_h, wo_h,
           inbox, logs, tokens, gain, wq, wk, wv, wf, bias, key, value, gate, wo,
           proj, pval, stats, acc, outs,
           in_sem, proj_s, proj_r, pval_s, pval_r, stats_s, stats_r, acc_s, acc_r, out_s, out_r):
    me = lax.axis_index("kv")
    mt = lax.axis_index("tp")
    batch, heads, positions = gate.shape
    width = wq.shape[1]
    size = width // heads

    pairs = [(tokens_h, tokens), (gain_h, gain), (wq_h, wq), (wf_h, wf), (wv_h, wv), (wk_h, wk), (gate_h, gate),
             (bias_h, bias), (key_h, key), (value_h, value), (wo_h, wo)]
    copies = [pltpu.make_async_copy(a, b, in_sem.at[i]) for i, (a, b) in enumerate(pairs)]
    (c_tok, c_gain, c_wq, c_wf, c_wv, c_wk, c_gate, c_bias, c_key, c_value, c_wo) = copies
    barrier = pltpu.get_barrier_semaphore()
    for d in range(1, n):
        pl.semaphore_signal(barrier, inc=1, device_id={"kv": lax.rem(me + d, n)}, device_id_type=pl.DeviceIdType.MESH)
    for d in range(1, t):
        pl.semaphore_signal(barrier, inc=1, device_id={"tp": lax.rem(mt + d, t)}, device_id_type=pl.DeviceIdType.MESH)

    for c in (c_tok, c_gain, c_wq, c_wf):
        c.start()
    late = (c_wv, c_wk, c_gate, c_bias, c_key, c_value, c_wo)

    c_tok.wait()
    c_gain.wait()
    wide = tokens[...].astype(F32)
    scaled = (wide * gain[...]).astype(BF16)
    square = jnp.sum(wide * wide, axis=-1, keepdims=True)
    c_wq.wait()
    c_wf.wait()
    for c in late:
        c.start()
    proj[me, :, :width] = jnp.dot(scaled, wq[...], preferred_element_type=F32)
    proj[me, :, width:] = jnp.broadcast_to(square, (batch, 128))
    proj[me, :, width : width + heads] = lax.dot_general(
        scaled, wf[...], (((1,), (1,)), ((), ())), preferred_element_type=F32)
    pl.semaphore_wait(barrier, n - 1 + t - 1)
    proj_x = ("kv", me, n, proj, proj_s, proj_r)
    exchange(*proj_x)

    c_wv.wait()
    pval[me] = jnp.dot(scaled, wv[...], preferred_element_type=F32).astype(BF16)
    pval_x = ("kv", me, n, pval, pval_s, pval_r)
    exchange(*pval_x)
    c_wk.wait()
    part_key = jnp.dot(scaled, wk[...], preferred_element_type=F32)
    c_gate.wait()
    c_bias.wait()
    c_key.wait()

    arrived(*proj_x)
    summed = jnp.sum(proj[...], axis=0)
    rstd = lax.rsqrt(summed[:, width + heads : width + heads + 1] / features + EPS)
    query = (summed[:, :width] * rstd).astype(BF16).astype(F32)
    forget = summed[:, width : width + heads] * rstd + bias[...]
    log_gate = jnp.minimum(forget, 0.0) - jnp.log1p(jnp.exp(-jnp.abs(forget)))

    row = lax.broadcasted_iota(jnp.int32, (heads, width), 0)
    col = lax.broadcasted_iota(jnp.int32, (heads, width), 1)
    own = (col >= row * size) & (col < (row + 1) * size)
    place = me * positions + lax.broadcasted_iota(jnp.int32, (heads, positions), 1)
    h_row = lax.broadcasted_iota(jnp.int32, (heads, 128), 0)
    lane = lax.broadcasted_iota(jnp.int32, (heads, 128), 1)
    scale = size ** -0.5
    c_value.wait()
    rows, sums = [], []
    for b in range(batch):
        spread = jnp.where(own, query[b : b + 1, :], 0.0)
        score = lax.dot_general(spread.astype(BF16), key[b], (((1,), (1,)), ((), ())), preferred_element_type=F32) * scale
        g = gate[b]
        usable = place < lengths[b]
        score = jnp.where(usable, score - g, MASKED)
        top = jnp.max(score, axis=-1, keepdims=True)
        weights = jnp.where(usable, jnp.exp(score - top), 0.0)
        total = jnp.sum(weights, axis=-1, keepdims=True)
        last = jnp.sum(jnp.where(place == lengths[b] - 1, g, 0.0), axis=-1, keepdims=True)
        own_score = jnp.sum(spread * part_key[b : b + 1, :], axis=-1, keepdims=True)
        tile = jnp.where(lane == h_row, top, 0.0)
        tile = jnp.where(lane == h_row + heads, total, tile)
        tile = jnp.where(lane == h_row + 2 * heads, last, tile)
        tile = jnp.where(lane == h_row + 3 * heads, own_score, tile)
        sums.append(jnp.sum(tile, axis=0, keepdims=True))
        full = jnp.dot(weights.astype(BF16), value[b], preferred_element_type=F32)
        rows.append(jnp.sum(jnp.where(own, full, 0.0), axis=0, keepdims=True))
    stats[me] = jnp.concatenate(sums, axis=0)
    acc[me] = jnp.concatenate(rows, axis=0).astype(BF16)
    stats_x = ("kv", me, n, stats, stats_s, stats_r)
    acc_x = ("kv", me, n, acc, acc_s, acc_r)
    exchange(*stats_x)
    exchange(*acc_x)

    arrived(*pval_x)
    value_new = jnp.sum(pval[...].astype(F32), axis=0)
    arrived(*stats_x)
    st = stats[...]
    tops = st[:, :, :heads]
    cache_max = jnp.max(tops, axis=0)
    factor = jnp.exp(tops - cache_max[None])
    cache_sum = jnp.sum(factor * st[:, :, heads : 2 * heads], axis=0)
    gate_now = jnp.sum(st[:, :, 2 * heads : 3 * heads], axis=0) + log_gate
    self_score = jnp.sum(st[:, :, 3 * heads : 4 * heads], axis=0) * rstd * scale
    cache_top = cache_max + gate_now
    top = jnp.maximum(cache_top, self_score)
    cache_factor = jnp.exp(cache_top - top)
    self_factor = jnp.exp(self_score - top)
    total = cache_sum * cache_factor + self_factor
    logs[...] = top + jnp.log(total)
    inverse = 1.0 / total
    each = factor * (cache_factor * inverse)[None]
    coef = jnp.concatenate([each.reshape(n * batch, heads), self_factor * inverse * rstd], axis=0)
    wide_coef = jnp.dot(coef, own.astype(F32), precision=lax.Precision.HIGHEST, preferred_element_type=F32)
    arrived(*acc_x)
    attended = wide_coef[n * batch :] * value_new + jnp.sum(
        wide_coef[: n * batch].reshape(n, batch, width) * acc[...].astype(F32), axis=0)
    c_wo.wait()
    partial = jnp.dot(attended.astype(BF16), wo[...], preferred_element_type=F32).astype(BF16)
    cols = partial.shape[1] // t
    for i in range(t):
        outs[i] = partial[:, i * cols : (i + 1) * cols]
    for d in range(1, t):
        peer = lax.rem(mt + d, t)
        pltpu.make_async_remote_copy(
            src_ref=outs.at[peer], dst_ref=inbox.at[mt], send_sem=out_s.at[d - 1], recv_sem=out_r.at[d - 1],
            device_id={"tp": peer}, device_id_type=pl.DeviceIdType.MESH).start()
    inbox[mt] = outs[mt]
    left(*proj_x)
    left(*pval_x)
    left(*stats_x)
    left(*acc_x)
    for d in range(1, t):
        slot = lax.rem(mt + t - d, t)
        pltpu.make_async_remote_copy(
            src_ref=outs.at[slot], dst_ref=inbox.at[slot], send_sem=out_s.at[d - 1], recv_sem=out_r.at[d - 1],
            device_id={"tp": slot}, device_id_type=pl.DeviceIdType.MESH).wait()


def finish(inbox, logs, mixed, log_total):
    mixed[...] = jnp.sum(inbox[...].astype(F32), axis=0).astype(BF16)
    log_total[...] = logs[...]


def body(n, t, tokens, norm_gain, w_query, w_key, w_value, w_forget, forget_bias, key_cache, value_cache, gate_cache,
         lengths, w_out):
    batch = tokens.shape[0]
    heads = gate_cache.shape[1]
    width = w_query.shape[1]
    cols = w_out.shape[1] // t
    arrays = (tokens, norm_gain.reshape(1, -1), w_query, w_key, w_value, w_forget.T, forget_bias.reshape(1, -1),
              key_cache, value_cache, gate_cache, w_out)
    dma = pltpu.SemaphoreType.DMA
    vmem = pl.BlockSpec(memory_space=pltpu.VMEM)
    inbox, logs = pl.pallas_call(
        functools.partial(kernel, n, t, float(tokens.shape[1] * n)),
        out_shape=(
            jax.ShapeDtypeStruct((t, batch, cols), BF16),
            jax.ShapeDtypeStruct((batch, heads), F32),
        ),
        in_specs=[pl.BlockSpec(memory_space=pltpu.SMEM)] + [pl.BlockSpec(memory_space=pl.ANY)] * len(arrays),
        out_specs=(vmem, vmem),
        scratch_shapes=[pltpu.VMEM(a.shape, a.dtype) for a in arrays] + [
            pltpu.VMEM((n, batch, width + 128), F32),
            pltpu.VMEM((n, batch, width), BF16),
            pltpu.VMEM((n, batch, 128), F32),
            pltpu.VMEM((n, batch, width), BF16),
            pltpu.VMEM((t, batch, cols), BF16),
            dma((len(arrays),)),
        ] + [dma((n - 1,))] * 8 + [dma((t - 1,))] * 2,
        compiler_params=pltpu.CompilerParams(collective_id=0, has_side_effects=True),
    )(lengths, *arrays)
    return pl.pallas_call(
        finish,
        out_shape=(jax.ShapeDtypeStruct((batch, cols), BF16), jax.ShapeDtypeStruct((batch, heads), F32)),
        in_specs=[vmem, vmem],
        out_specs=(vmem, vmem),
    )(inbox, logs)


def solution(mesh):
    placed = (
        P(None, "kv"),
        P("kv"),
        P("kv", "tp"),
        P("kv", "tp"),
        P("kv", "tp"),
        P("kv", "tp"),
        P("tp"),
        P(None, "kv", "tp"),
        P(None, "kv", "tp"),
        P(None, "tp", "kv"),
        P(),
        P("tp", "kv"),
    )
    return jax.shard_map(
        functools.partial(body, mesh.shape["kv"], mesh.shape["tp"]),
        mesh=mesh,
        in_specs=placed,
        out_specs=(P(None, ("kv", "tp")), P(None, "tp")),
        check_vma=False,
    )
```

```python
import functools

import jax
import jax.numpy as jnp
from jax import lax
from jax.experimental import pallas as pl
from jax.experimental.pallas import tpu as pltpu
from jax.sharding import PartitionSpec as P

EPS = 1e-06
MASKED = -1e30
F32 = jnp.float32
BF16 = jnp.bfloat16


def exchange(axis, me, n, buf, send_sem, recv_sem):
    for d in sorted(range(1, n), key=lambda d: -min(d, n - d)):
        pltpu.make_async_remote_copy(
            src_ref=buf.at[me],
            dst_ref=buf.at[me],
            send_sem=send_sem.at[d - 1],
            recv_sem=recv_sem.at[d - 1],
            device_id={axis: lax.rem(me + d, n)},
            device_id_type=pl.DeviceIdType.MESH,
        ).start()


def arrived(axis, me, n, buf, send_sem, recv_sem):
    for d in range(1, n):
        slot = lax.rem(me + n - d, n)
        pltpu.make_async_remote_copy(
            src_ref=buf.at[slot],
            dst_ref=buf.at[slot],
            send_sem=send_sem.at[d - 1],
            recv_sem=recv_sem.at[d - 1],
            device_id={axis: slot},
            device_id_type=pl.DeviceIdType.MESH,
        ).wait_recv()


def left(axis, me, n, buf, send_sem, recv_sem):
    for d in range(1, n):
        pltpu.make_async_remote_copy(
            src_ref=buf.at[me],
            dst_ref=buf.at[me],
            send_sem=send_sem.at[d - 1],
            recv_sem=recv_sem.at[d - 1],
            device_id={axis: lax.rem(me + d, n)},
            device_id_type=pl.DeviceIdType.MESH,
        ).wait_send()


def kernel(n, t, features, lengths, tokens_h, gain_h, wq_h, wk_h, wv_h, wf_h, bias_h, key_h, value_h, gate_h, wo_h,
           inbox, logs, tokens, gain, wq, wk, wv, wf, bias, key, value, gate, wo,
           proj, pval, stats, acc, outs,
           in_sem, proj_s, proj_r, pval_s, pval_r, stats_s, stats_r, acc_s, acc_r, out_s, out_r):
    me = lax.axis_index("kv")
    mt = lax.axis_index("tp")
    batch, heads, positions = gate.shape
    width = wq.shape[1]
    size = width // heads

    pairs = [(tokens_h, tokens), (gain_h, gain), (wq_h, wq), (wf_h, wf), (wv_h, wv), (wk_h, wk), (gate_h, gate),
             (bias_h, bias), (key_h, key), (value_h, value), (wo_h, wo)]
    copies = [pltpu.make_async_copy(a, b, in_sem.at[i]) for i, (a, b) in enumerate(pairs)]
    (c_tok, c_gain, c_wq, c_wf, c_wv, c_wk, c_gate, c_bias, c_key, c_value, c_wo) = copies
    barrier = pltpu.get_barrier_semaphore()
    for d in range(1, n):
        pl.semaphore_signal(barrier, inc=1, device_id={"kv": lax.rem(me + d, n)}, device_id_type=pl.DeviceIdType.MESH)
    for d in range(1, t):
        pl.semaphore_signal(barrier, inc=1, device_id={"tp": lax.rem(mt + d, t)}, device_id_type=pl.DeviceIdType.MESH)

    for c in (c_tok, c_gain, c_wq, c_wf):
        c.start()
    late = (c_wv, c_wk, c_gate, c_bias, c_key, c_value, c_wo)

    c_tok.wait()
    c_gain.wait()
    wide = tokens[...].astype(F32)
    scaled = (wide * gain[...]).astype(BF16)
    square = jnp.sum(wide * wide, axis=-1, keepdims=True)
    c_wq.wait()
    c_wf.wait()
    for c in late:
        c.start()
    proj[me, :, :width] = jnp.dot(scaled, wq[...], preferred_element_type=F32)
    proj[me, :, width:] = jnp.broadcast_to(square, (batch, 128))
    proj[me, :, width : width + heads] = lax.dot_general(
        scaled, wf[...], (((1,), (1,)), ((), ())), preferred_element_type=F32)
    pl.semaphore_wait(barrier, n - 1 + t - 1)
    proj_x = ("kv", me, n, proj, proj_s, proj_r)
    exchange(*proj_x)

    c_wv.wait()
    pval[me] = jnp.dot(scaled, wv[...], preferred_element_type=F32).astype(BF16)
    pval_x = ("kv", me, n, pval, pval_s, pval_r)
    c_wk.wait()
    part_key = jnp.dot(scaled, wk[...], preferred_element_type=F32)
    c_gate.wait()
    c_bias.wait()
    c_key.wait()

    arrived(*proj_x)
    exchange(*pval_x)
    summed = jnp.sum(proj[...], axis=0)
    rstd = lax.rsqrt(summed[:, width + heads : width + heads + 1] / features + EPS)
    query = (summed[:, :width] * rstd).astype(BF16).astype(F32)
    forget = summed[:, width : width + heads] * rstd + bias[...]
    log_gate = jnp.minimum(forget, 0.0) - jnp.log1p(jnp.exp(-jnp.abs(forget)))

    row = lax.broadcasted_iota(jnp.int32, (heads, width), 0)
    col = lax.broadcasted_iota(jnp.int32, (heads, width), 1)
    own = (col >= row * size) & (col < (row + 1) * size)
    place = me * positions + lax.broadcasted_iota(jnp.int32, (heads, positions), 1)
    h_row = lax.broadcasted_iota(jnp.int32, (heads, 128), 0)
    lane = lax.broadcasted_iota(jnp.int32, (heads, 128), 1)
    scale = size ** -0.5
    rows, sums, lows = [], [], []
    for b in range(batch):
        spread = jnp.where(own, query[b : b + 1, :], 0.0)
        score = lax.dot_general(spread.astype(BF16), key[b], (((1,), (1,)), ((), ())), preferred_element_type=F32) * scale
        g = gate[b]
        usable = place < lengths[b]
        score = jnp.where(usable, score - g, MASKED)
        top = jnp.max(score, axis=-1, keepdims=True)
        weights = jnp.where(usable, jnp.exp(score - top), 0.0)
        total = jnp.sum(weights, axis=-1, keepdims=True)
        last = jnp.sum(jnp.where(place == lengths[b] - 1, g, 0.0), axis=-1, keepdims=True)
        own_score = jnp.sum(spread * part_key[b : b + 1, :], axis=-1, keepdims=True)
        tile = jnp.where(lane == h_row, top, 0.0)
        tile = jnp.where(lane == h_row + heads, total, tile)
        tile = jnp.where(lane == h_row + 2 * heads, last, tile)
        tile = jnp.where(lane == h_row + 3 * heads, own_score, tile)
        sums.append(jnp.sum(tile, axis=0, keepdims=True))
        lows.append(weights.astype(BF16))
    stats[me] = jnp.concatenate(sums, axis=0)
    stats_x = ("kv", me, n, stats, stats_s, stats_r)
    exchange(*stats_x)
    c_value.wait()
    for b in range(batch):
        full = jnp.dot(lows[b], value[b], preferred_element_type=F32)
        rows.append(jnp.sum(jnp.where(own, full, 0.0), axis=0, keepdims=True))
    acc[me] = jnp.concatenate(rows, axis=0).astype(BF16)
    acc_x = ("kv", me, n, acc, acc_s, acc_r)
    exchange(*acc_x)

    arrived(*pval_x)
    value_new = jnp.sum(pval[...].astype(F32), axis=0)
    arrived(*stats_x)
    st = stats[...]
    tops = st[:, :, :heads]
    cache_max = jnp.max(tops, axis=0)
    factor = jnp.exp(tops - cache_max[None])
    cache_sum = jnp.sum(factor * st[:, :, heads : 2 * heads], axis=0)
    gate_now = jnp.sum(st[:, :, 2 * heads : 3 * heads], axis=0) + log_gate
    self_score = jnp.sum(st[:, :, 3 * heads : 4 * heads], axis=0) * rstd * scale
    cache_top = cache_max + gate_now
    top = jnp.maximum(cache_top, self_score)
    cache_factor = jnp.exp(cache_top - top)
    self_factor = jnp.exp(self_score - top)
    total = cache_sum * cache_factor + self_factor
    logs[...] = top + jnp.log(total)
    inverse = 1.0 / total
    each = factor * (cache_factor * inverse)[None]
    coef = jnp.concatenate([each.reshape(n * batch, heads), self_factor * inverse * rstd], axis=0)
    wide_coef = jnp.dot(coef, own.astype(F32), precision=lax.Precision.HIGHEST, preferred_element_type=F32)
    arrived(*acc_x)
    attended = wide_coef[n * batch :] * value_new + jnp.sum(
        wide_coef[: n * batch].reshape(n, batch, width) * acc[...].astype(F32), axis=0)
    c_wo.wait()
    partial = jnp.dot(attended.astype(BF16), wo[...], preferred_element_type=F32).astype(BF16)
    cols = partial.shape[1] // t
    for i in range(t):
        outs[i] = partial[:, i * cols : (i + 1) * cols]
    for d in range(1, t):
        peer = lax.rem(mt + d, t)
        pltpu.make_async_remote_copy(
            src_ref=outs.at[peer], dst_ref=inbox.at[mt], send_sem=out_s.at[d - 1], recv_sem=out_r.at[d - 1],
            device_id={"tp": peer}, device_id_type=pl.DeviceIdType.MESH).start()
    inbox[mt] = outs[mt]
    left(*proj_x)
    left(*pval_x)
    left(*stats_x)
    left(*acc_x)
    for d in range(1, t):
        slot = lax.rem(mt + t - d, t)
        pltpu.make_async_remote_copy(
            src_ref=outs.at[slot], dst_ref=inbox.at[slot], send_sem=out_s.at[d - 1], recv_sem=out_r.at[d - 1],
            device_id={"tp": slot}, device_id_type=pl.DeviceIdType.MESH).wait()


def finish(inbox, logs, mixed, log_total):
    mixed[...] = jnp.sum(inbox[...].astype(F32), axis=0).astype(BF16)
    log_total[...] = logs[...]


def body(n, t, tokens, norm_gain, w_query, w_key, w_value, w_forget, forget_bias, key_cache, value_cache, gate_cache,
         lengths, w_out):
    batch = tokens.shape[0]
    heads = gate_cache.shape[1]
    width = w_query.shape[1]
    cols = w_out.shape[1] // t
    arrays = (tokens, norm_gain.reshape(1, -1), w_query, w_key, w_value, w_forget.T, forget_bias.reshape(1, -1),
              key_cache, value_cache, gate_cache, w_out)
    dma = pltpu.SemaphoreType.DMA
    vmem = pl.BlockSpec(memory_space=pltpu.VMEM)
    inbox, logs = pl.pallas_call(
        functools.partial(kernel, n, t, float(tokens.shape[1] * n)),
        out_shape=(
            jax.ShapeDtypeStruct((t, batch, cols), BF16),
            jax.ShapeDtypeStruct((batch, heads), F32),
        ),
        in_specs=[pl.BlockSpec(memory_space=pltpu.SMEM)] + [pl.BlockSpec(memory_space=pl.ANY)] * len(arrays),
        out_specs=(vmem, vmem),
        scratch_shapes=[pltpu.VMEM(a.shape, a.dtype) for a in arrays] + [
            pltpu.VMEM((n, batch, width + 128), F32),
            pltpu.VMEM((n, batch, width), BF16),
            pltpu.VMEM((n, batch, 128), F32),
            pltpu.VMEM((n, batch, width), BF16),
            pltpu.VMEM((t, batch, cols), BF16),
            dma((len(arrays),)),
        ] + [dma((n - 1,))] * 8 + [dma((t - 1,))] * 2,
        compiler_params=pltpu.CompilerParams(collective_id=0, has_side_effects=True),
    )(lengths, *arrays)
    return pl.pallas_call(
        finish,
        out_shape=(jax.ShapeDtypeStruct((batch, cols), BF16), jax.ShapeDtypeStruct((batch, heads), F32)),
        in_specs=[vmem, vmem],
        out_specs=(vmem, vmem),
    )(inbox, logs)


def solution(mesh):
    placed = (
        P(None, "kv"),
        P("kv"),
        P("kv", "tp"),
        P("kv", "tp"),
        P("kv", "tp"),
        P("kv", "tp"),
        P("tp"),
        P(None, "kv", "tp"),
        P(None, "kv", "tp"),
        P(None, "tp", "kv"),
        P(),
        P("tp", "kv"),
    )
    return jax.shard_map(
        functools.partial(body, mesh.shape["kv"], mesh.shape["tp"]),
        mesh=mesh,
        in_specs=placed,
        out_specs=(P(None, ("kv", "tp")), P(None, "tp")),
        check_vma=False,
    )
```

```python
import functools

import jax
import jax.numpy as jnp
from jax import lax
from jax.experimental import pallas as pl
from jax.experimental.pallas import tpu as pltpu
from jax.sharding import PartitionSpec as P

EPS = 1e-06
MASKED = -1e30
F32 = jnp.float32
BF16 = jnp.bfloat16


def exchange(axis, me, n, buf, send_sem, recv_sem):
    for d in sorted(range(1, n), key=lambda d: -min(d, n - d)):
        pltpu.make_async_remote_copy(
            src_ref=buf.at[me],
            dst_ref=buf.at[me],
            send_sem=send_sem.at[d - 1],
            recv_sem=recv_sem.at[d - 1],
            device_id={axis: lax.rem(me + d, n)},
            device_id_type=pl.DeviceIdType.MESH,
        ).start()


def arrived(axis, me, n, buf, send_sem, recv_sem):
    for d in range(1, n):
        slot = lax.rem(me + n - d, n)
        pltpu.make_async_remote_copy(
            src_ref=buf.at[slot],
            dst_ref=buf.at[slot],
            send_sem=send_sem.at[d - 1],
            recv_sem=recv_sem.at[d - 1],
            device_id={axis: slot},
            device_id_type=pl.DeviceIdType.MESH,
        ).wait_recv()


def left(axis, me, n, buf, send_sem, recv_sem):
    for d in range(1, n):
        pltpu.make_async_remote_copy(
            src_ref=buf.at[me],
            dst_ref=buf.at[me],
            send_sem=send_sem.at[d - 1],
            recv_sem=recv_sem.at[d - 1],
            device_id={axis: lax.rem(me + d, n)},
            device_id_type=pl.DeviceIdType.MESH,
        ).wait_send()


def kernel(n, t, features, lengths, tokens_h, gain_h, wq_h, wk_h, wv_h, wf_h, bias_h, key_h, value_h, gate_h, wo_h,
           inbox, logs, tokens, gain, wq, wk, wv, wf, bias, key, value, gate, wo,
           proj, pval, stats, acc, outs,
           in_sem, proj_s, proj_r, pval_s, pval_r, stats_s, stats_r, acc_s, acc_r, out_s, out_r):
    me = lax.axis_index("kv")
    mt = lax.axis_index("tp")
    batch, heads, positions = gate.shape
    width = wq.shape[1]
    size = width // heads

    pairs = [(tokens_h, tokens), (gain_h, gain), (wq_h, wq), (wf_h, wf), (wv_h, wv), (wk_h, wk), (gate_h, gate),
             (bias_h, bias), (key_h, key), (value_h, value), (wo_h, wo)]
    copies = [pltpu.make_async_copy(a, b, in_sem.at[i]) for i, (a, b) in enumerate(pairs)]
    (c_tok, c_gain, c_wq, c_wf, c_wv, c_wk, c_gate, c_bias, c_key, c_value, c_wo) = copies
    barrier = pltpu.get_barrier_semaphore()
    for d in range(1, n):
        pl.semaphore_signal(barrier, inc=1, device_id={"kv": lax.rem(me + d, n)}, device_id_type=pl.DeviceIdType.MESH)
    for d in range(1, t):
        pl.semaphore_signal(barrier, inc=1, device_id={"tp": lax.rem(mt + d, t)}, device_id_type=pl.DeviceIdType.MESH)

    for c in (c_tok, c_gain, c_wq, c_wf):
        c.start()
    late = (c_wv, c_wk, c_gate, c_bias, c_key, c_value, c_wo)

    c_tok.wait()
    c_gain.wait()
    wide = tokens[...].astype(F32)
    scaled = (wide * gain[...]).astype(BF16)
    square = jnp.sum(wide * wide, axis=-1, keepdims=True)
    c_wq.wait()
    c_wf.wait()
    for c in late:
        c.start()
    proj[me, :, :width] = jnp.dot(scaled, wq[...], preferred_element_type=F32)
    proj[me, :, width:] = jnp.broadcast_to(square, (batch, 128))
    proj[me, :, width : width + heads] = lax.dot_general(
        scaled, wf[...], (((1,), (1,)), ((), ())), preferred_element_type=F32)
    pl.semaphore_wait(barrier, n - 1 + t - 1)
    proj_x = ("kv", me, n, proj, proj_s, proj_r)
    exchange(*proj_x)

    c_wv.wait()
    pval[me] = jnp.dot(scaled, wv[...], preferred_element_type=F32).astype(BF16)
    pval_x = ("kv", me, n, pval, pval_s, pval_r)
    c_wk.wait()
    part_key = jnp.dot(scaled, wk[...], preferred_element_type=F32)
    c_gate.wait()
    c_bias.wait()
    c_key.wait()
    row = lax.broadcasted_iota(jnp.int32, (heads, width), 0)
    col = lax.broadcasted_iota(jnp.int32, (heads, width), 1)
    own = (col >= row * size) & (col < (row + 1) * size)
    place = me * positions + lax.broadcasted_iota(jnp.int32, (heads, positions), 1)
    h_row = lax.broadcasted_iota(jnp.int32, (heads, 128), 0)
    lane = lax.broadcasted_iota(jnp.int32, (heads, 128), 1)
    scale = size ** -0.5
    lasts = [
        jnp.sum(jnp.where(place == lengths[b] - 1, gate[b], 0.0), axis=-1, keepdims=True) for b in range(batch)
    ]

    arrived(*proj_x)
    exchange(*pval_x)
    summed = jnp.sum(proj[...], axis=0)
    rstd = lax.rsqrt(summed[:, width + heads : width + heads + 1] / features + EPS)
    query = (summed[:, :width] * rstd).astype(BF16).astype(F32)
    forget = summed[:, width : width + heads] * rstd + bias[...]
    log_gate = jnp.minimum(forget, 0.0) - jnp.log1p(jnp.exp(-jnp.abs(forget)))

    rows, sums, lows = [], [], []
    spreads = [jnp.where(own, query[b : b + 1, :], 0.0) for b in range(batch)]
    scores = [
        lax.dot_general(spreads[b].astype(BF16), key[b], (((1,), (1,)), ((), ())), preferred_element_type=F32) * scale
        for b in range(batch)
    ]
    for b in range(batch):
        spread, score = spreads[b], scores[b]
        g = gate[b]
        usable = place < lengths[b]
        score = jnp.where(usable, score - g, MASKED)
        top = jnp.max(score, axis=-1, keepdims=True)
        weights = jnp.where(usable, jnp.exp(score - top), 0.0)
        total = jnp.sum(weights, axis=-1, keepdims=True)
        own_score = jnp.sum(spread * part_key[b : b + 1, :], axis=-1, keepdims=True)
        tile = jnp.where(lane == h_row, top, 0.0)
        tile = jnp.where(lane == h_row + heads, total, tile)
        tile = jnp.where(lane == h_row + 2 * heads, lasts[b], tile)
        tile = jnp.where(lane == h_row + 3 * heads, own_score, tile)
        sums.append(jnp.sum(tile, axis=0, keepdims=True))
        lows.append(weights.astype(BF16))
    stats[me] = jnp.concatenate(sums, axis=0)
    stats_x = ("kv", me, n, stats, stats_s, stats_r)
    exchange(*stats_x)
    c_value.wait()
    for b in range(batch):
        full = jnp.dot(lows[b], value[b], preferred_element_type=F32)
        rows.append(jnp.sum(jnp.where(own, full, 0.0), axis=0, keepdims=True))
    acc[me] = jnp.concatenate(rows, axis=0).astype(BF16)
    acc_x = ("kv", me, n, acc, acc_s, acc_r)
    exchange(*acc_x)

    arrived(*pval_x)
    value_new = jnp.sum(pval[...].astype(F32), axis=0)
    arrived(*stats_x)
    st = stats[...]
    tops = st[:, :, :heads]
    cache_max = jnp.max(tops, axis=0)
    factor = jnp.exp(tops - cache_max[None])
    cache_sum = jnp.sum(factor * st[:, :, heads : 2 * heads], axis=0)
    gate_now = jnp.sum(st[:, :, 2 * heads : 3 * heads], axis=0) + log_gate
    self_score = jnp.sum(st[:, :, 3 * heads : 4 * heads], axis=0) * rstd * scale
    cache_top = cache_max + gate_now
    top = jnp.maximum(cache_top, self_score)
    cache_factor = jnp.exp(cache_top - top)
    self_factor = jnp.exp(self_score - top)
    total = cache_sum * cache_factor + self_factor
    logs[...] = top + jnp.log(total)
    inverse = 1.0 / total
    each = factor * (cache_factor * inverse)[None]
    coef = jnp.concatenate([each.reshape(n * batch, heads), self_factor * inverse * rstd], axis=0)
    wide_coef = jnp.dot(coef, own.astype(F32), precision=lax.Precision.HIGHEST, preferred_element_type=F32)
    arrived(*acc_x)
    attended = wide_coef[n * batch :] * value_new + jnp.sum(
        wide_coef[: n * batch].reshape(n, batch, width) * acc[...].astype(F32), axis=0)
    c_wo.wait()
    partial = jnp.dot(attended.astype(BF16), wo[...], preferred_element_type=F32).astype(BF16)
    cols = partial.shape[1] // t
    for i in range(t):
        outs[i] = partial[:, i * cols : (i + 1) * cols]
    for d in range(1, t):
        peer = lax.rem(mt + d, t)
        pltpu.make_async_remote_copy(
            src_ref=outs.at[peer], dst_ref=inbox.at[mt], send_sem=out_s.at[d - 1], recv_sem=out_r.at[d - 1],
            device_id={"tp": peer}, device_id_type=pl.DeviceIdType.MESH).start()
    inbox[mt] = outs[mt]
    left(*proj_x)
    left(*pval_x)
    left(*stats_x)
    left(*acc_x)
    for d in range(1, t):
        slot = lax.rem(mt + t - d, t)
        pltpu.make_async_remote_copy(
            src_ref=outs.at[slot], dst_ref=inbox.at[slot], send_sem=out_s.at[d - 1], recv_sem=out_r.at[d - 1],
            device_id={"tp": slot}, device_id_type=pl.DeviceIdType.MESH).wait()


def finish(inbox, logs, mixed, log_total):
    mixed[...] = jnp.sum(inbox[...].astype(F32), axis=0).astype(BF16)
    log_total[...] = logs[...]


def body(n, t, tokens, norm_gain, w_query, w_key, w_value, w_forget, forget_bias, key_cache, value_cache, gate_cache,
         lengths, w_out):
    batch = tokens.shape[0]
    heads = gate_cache.shape[1]
    width = w_query.shape[1]
    cols = w_out.shape[1] // t
    arrays = (tokens, norm_gain.reshape(1, -1), w_query, w_key, w_value, w_forget.T, forget_bias.reshape(1, -1),
              key_cache, value_cache, gate_cache, w_out)
    dma = pltpu.SemaphoreType.DMA
    vmem = pl.BlockSpec(memory_space=pltpu.VMEM)
    inbox, logs = pl.pallas_call(
        functools.partial(kernel, n, t, float(tokens.shape[1] * n)),
        out_shape=(
            jax.ShapeDtypeStruct((t, batch, cols), BF16),
            jax.ShapeDtypeStruct((batch, heads), F32),
        ),
        in_specs=[pl.BlockSpec(memory_space=pltpu.SMEM)] + [pl.BlockSpec(memory_space=pl.ANY)] * len(arrays),
        out_specs=(vmem, vmem),
        scratch_shapes=[pltpu.VMEM(a.shape, a.dtype) for a in arrays] + [
            pltpu.VMEM((n, batch, width + 128), F32),
            pltpu.VMEM((n, batch, width), BF16),
            pltpu.VMEM((n, batch, 128), F32),
            pltpu.VMEM((n, batch, width), BF16),
            pltpu.VMEM((t, batch, cols), BF16),
            dma((len(arrays),)),
        ] + [dma((n - 1,))] * 8 + [dma((t - 1,))] * 2,
        compiler_params=pltpu.CompilerParams(collective_id=0, has_side_effects=True),
    )(lengths, *arrays)
    return pl.pallas_call(
        finish,
        out_shape=(jax.ShapeDtypeStruct((batch, cols), BF16), jax.ShapeDtypeStruct((batch, heads), F32)),
        in_specs=[vmem, vmem],
        out_specs=(vmem, vmem),
    )(inbox, logs)


def solution(mesh):
    placed = (
        P(None, "kv"),
        P("kv"),
        P("kv", "tp"),
        P("kv", "tp"),
        P("kv", "tp"),
        P("kv", "tp"),
        P("tp"),
        P(None, "kv", "tp"),
        P(None, "kv", "tp"),
        P(None, "tp", "kv"),
        P(),
        P("tp", "kv"),
    )
    return jax.shard_map(
        functools.partial(body, mesh.shape["kv"], mesh.shape["tp"]),
        mesh=mesh,
        in_specs=placed,
        out_specs=(P(None, ("kv", "tp")), P(None, "tp")),
        check_vma=False,
    )
```
